32 devices in a mesh: grp: 2 (over y), ep: 4 (over z), tp: 4 (over x, core).
Axes of the slice: x: 2, y: 2, z: 4, core: 2. Of those that a mesh axis runs over, the one named last changes fastest.
Arguments:
- memory_query_rows: bfloat16 [1024, 1024], P(('grp', 'ep'), 'tp'), parts along dimension 0, may hold values from -6 to 6
- memory_key_rows: bfloat16 [1024, 1024], P(('grp', 'ep'), 'tp'), parts along dimension 0, may hold values from -6 to 6
- memory_value_rows: bfloat16 [1024, 1024], P(('grp', 'ep'), 'tp'), parts along dimension 0, may hold values from -6 to 6
- input_gate_log: float32 [8, 1024], P('tp', ('grp', 'ep')), parts along dimension 1, may hold values from -4 to 300
- forget_gate_logits: float32 [8, 1024], P('tp', ('grp', 'ep')), parts along dimension 1
- forget_log_extra: float32 [8, 1024], P('tp', ('grp', 'ep')), parts along dimension 1, may hold values from -1.5 to 0
- memory_output_weight: bfloat16 [1024, 2048], P(None, 'tp'), may hold values from -0.1875 to 0.1875
- second_batch_tokens: bfloat16 [4096, 2048], P(('grp', 'ep', 'tp')), parts along dimension 0, may hold values from -6 to 6
- expert_norm_gain: float32 [2048], replicated, may hold values from 0.1 to 1.9
- routing_expert_index: int32 [4096, 2], P(('grp', 'ep', 'tp')), parts along dimension 0, may hold values from 0 to 3, all different within a row; in each aligned block of 128 rows (0 to 127, 128 to 255, ...) at most 80 rows name the same one
- routing_expert_weight: float32 [4096, 2], P(('grp', 'ep', 'tp')), parts along dimension 0, may hold values from 0.2 to 1
- expert_gate_matrix: bfloat16 [4, 2048, 3584], P('ep', None, 'tp'), may hold values from -0.125 to 0.125
- expert_up_matrix: bfloat16 [4, 2048, 3584], P('ep', None, 'tp'), may hold values from -0.125 to 0.125
- expert_down_matrix: bfloat16 [4, 3584, 2048], P('ep', 'tp'), may hold values from -0.09375 to 0.09375
Outputs:
- mixed_out: bfloat16 [1024, 2048], P(('grp', 'ep'), 'tp'), parts along dimension 0
- expert_out: bfloat16 [4096, 2048], P(('grp', 'ep', 'tp')), parts along dimension 0
The draws below stay inside these ranges and needn't reach their ends.
There are 2 independent parts, one for each index of `grp`. The reference program is written for one: setup_inputs(seed, part) draws one part's arguments, and reference() takes and returns one part's arrays. A program takes and returns all parts, laid end to end along the dimension named above; an argument that names none is the same for every part. Nothing has to cross between parts.
Inputs may be any that keep to these rules, and one draw needn't show every extreme that they name: `routing_expert_index`: within the rows of one device no expert is named by more than 80 rows, a bound that some block reaches; the 2 experts of a row differ.
All inputs are finite; a program needn't handle non-finite values.
Results may differ from the reference program's by a relative error of at most 0.012.
The reference program's roundings to bfloat16 on the way count: a program that leaves them out, or rounds other values in their place, can miss the bound.
Values may be sent and summed in bfloat16 or wider, within the bound.
A program may use at most 128 MiB of HBM per device.

```python
import math
import jax
import jax.numpy as jnp
import numpy as np
from jax import lax

D = 2048
HM = 8
DH = 128
FFE = 3584
TOP = 2
BLOCK = 128
TOK_A_EP = 128
TOK_B_DEV = 128
SEQ_LEN = 512
TOKENS_B = 2048
EXPERTS = 4
CAP = 80
N_TP = 4


def draw_input_gate_log(key, part):
    keys = jax.random.split(key, 1)
    base = jax.random.truncated_normal(keys[0], -4.0, 4.0, (HM, SEQ_LEN), jnp.float32)
    return base.astype(jnp.float32)


def draw_forget_gate_logits(key, part):
    keys = jax.random.split(key, 4)
    threshold = 0.5
    fast = jax.random.uniform(keys[0], (HM,), jnp.float32) < threshold
    fast_rate = 1.0 / jax.random.uniform(keys[1], (HM,), jnp.float32, 30.0, 100.0)
    slow_rate = 0.3 / SEQ_LEN
    rate = jnp.where(fast, fast_rate, slow_rate)
    factor = jnp.exp(jax.random.uniform(keys[2], (HM, SEQ_LEN // TOK_A_EP), jnp.float32, -0.7, 0.7))
    factor = jnp.repeat(factor, TOK_A_EP, axis=1)
    noise = 0.5 * jax.random.truncated_normal(keys[3], -4.0, 4.0, (HM, SEQ_LEN), jnp.float32)
    return (-jnp.log(jnp.expm1(rate[:, None] * factor)) + noise).astype(jnp.float32)


def draw_forget_log_extra(key, part):
    keys = jax.random.split(key, 2)
    places = jax.random.randint(keys[0], (HM, 3), 0, SEQ_LEN)
    amounts = jnp.log(jax.random.uniform(keys[1], (HM, 3), jnp.float32, 0.5, 0.8))
    spots = jnp.arange(SEQ_LEN, dtype=jnp.int32)[None, :]
    result = jnp.zeros((HM, SEQ_LEN), jnp.float32)
    for column in range(3):
        result = result + jnp.where(spots == places[:, column:column + 1], amounts[:, column:column + 1], 0.0)
    return result.astype(jnp.float32)


def block_levels(own_key, shape, cuts, low, top_value):
    loudness, own = 1.0, jax.random.fold_in(own_key, 6)
    for axis_at, parts in cuts:
        draws = jnp.exp(jax.random.uniform(jax.random.fold_in(own, axis_at), (parts,), jnp.float32, low / len(cuts), top_value / len(cuts)))
        loudness = loudness * jnp.repeat(draws, shape[axis_at] // parts).reshape([-1 if axis == axis_at else 1 for axis in range(len(shape))])
    return loudness


def shared_out(own_key, own, number, rows, amount, top, reach, lean):
    sequence = jax.random.permutation(own_key, amount)
    packed, usual = load_shares(amount, rows * top, reach, lean, True), load_shares(amount, rows * top, reach, lean, False)
    places = jnp.arange(amount)

    def named(lengths, offset_by):
        used = int((lengths > 0).sum())
        fixed = max(1, used // 4)
        passed = fixed + (places - fixed + offset_by * (used - fixed)) % max(1, amount - fixed)
        return jnp.zeros((amount,), jnp.int32).at[sequence[jnp.where(places < fixed, places, passed)]].set(jnp.asarray(lengths, jnp.int32))

    lengths = jnp.where(number % 4 == 0, named(packed, number // 4), named(usual, number - number // 4 - 1))
    mixed = jax.random.permutation(jax.random.fold_in(own, 3), amount)
    giver, sink = mixed[0:amount // 2 * 2:2], mixed[1:amount // 2 * 2:2]
    margin = jnp.minimum(lengths[giver] - 1, reach - lengths[sink]) // 2
    margin = jnp.where((giver == sequence[0]) | (sink == sequence[0]) | (lengths[sink] == 0), 0, jnp.maximum(margin, 0))
    passed = jax.random.randint(jax.random.fold_in(own, 4), (amount // 2,), 0, 1 << 20) % (margin + 1)
    lengths = lengths.at[giver].add(-passed).at[sink].add(passed)
    items = jnp.searchsorted(jnp.cumsum(lengths), jnp.arange(rows * top), side="right").astype(jnp.int32)
    grid = items.reshape(top, rows).T
    grid = grid[jax.random.permutation(jax.random.fold_in(own, 1), rows)]
    offset_by = jax.random.randint(jax.random.fold_in(own, 2), (rows, 1), 0, top)
    return jnp.take_along_axis(grid, (jnp.arange(top)[None, :] + offset_by) % top, axis=1)


def load_shares(count, total, reach, lean, full):
    loads = [(1 << 20) // math.isqrt(rank ** lean) + 1 for rank in range(1, count + 1)]
    largest = reach if full else min(reach, max(-(-total // count), total * loads[0] // sum(loads)))
    least = 1 if total - largest >= count - 1 else 0
    given, spare = [largest] + [least] * (count - 1), total - largest - least * (count - 1)
    while spare > 0:
        free = [i for i in range(1, count) if given[i] < largest] or [i for i in range(1, count) if given[i] < reach]
        whole, left = sum([loads[i] for i in free]), spare
        for i in free:
            addition = min(reach - given[i], max(1, left * loads[i] // whole), spare)
            given[i] = given[i] + addition
            spare = spare - addition
    return np.array(given)


def bell_draw(key, dims, scale, bound, pieces=(), held_as=jnp.bfloat16):
    values = jax.random.normal(key, dims, jnp.float32) * scale
    if len(pieces) > 0:
        values = block_levels(key, dims, pieces, -0.22, 0.18) * values
    return jnp.clip(values, min=-bound, max=bound).astype(held_as)


def setup_inputs(seed: int = 0, part: int = 0) -> dict:
    seeds = jax.random.split(jax.random.key(seed), 15)
    part_splits = jax.random.split(jax.random.fold_in(seeds[14], part), 15)
    memory_query_rows = bell_draw(part_splits[0], (SEQ_LEN, HM * DH), 1.0, 6.0, ((0, 4), (1, 4)))
    memory_key_rows = bell_draw(part_splits[1], (SEQ_LEN, HM * DH), 1.0, 6.0, ((0, 4), (1, 4)))
    memory_value_rows = bell_draw(part_splits[2], (SEQ_LEN, HM * DH), 1.0, 6.0, ((0, 4), (1, 4)))
    input_gate_log = draw_input_gate_log(jax.random.fold_in(jax.random.fold_in(seeds[14], part), 71), part)
    forget_gate_logits = draw_forget_gate_logits(jax.random.fold_in(jax.random.fold_in(seeds[14], part), 71), part)
    forget_log_extra = draw_forget_log_extra(jax.random.fold_in(jax.random.fold_in(seeds[14], part), 71), part)
    memory_output_weight = bell_draw(seeds[6], (HM * DH, D), (HM * DH) ** -0.5, 0.1875, ((1, 4),))
    second_batch_tokens = bell_draw(part_splits[7], (TOKENS_B, D), 1.0, 6.0, ((0, 16),))
    expert_norm_gain = jnp.clip(1.0 + 0.18 * jax.random.normal(seeds[8], (D,), jnp.float32), 0.1, 1.9)
    routing_expert_index_keys = jax.random.split(jax.random.fold_in(part_splits[9], 1), TOKENS_B // TOK_B_DEV)
    routing_expert_index_turns = jax.random.permutation(jax.random.fold_in(part_splits[9], 3), TOKENS_B // TOK_B_DEV)
    routing_expert_index = jax.vmap(lambda own, number: shared_out(jax.random.fold_in(part_splits[9], 2), own, number, TOK_B_DEV, EXPERTS, TOP, CAP, 1))(routing_expert_index_keys, routing_expert_index_turns).reshape((TOKENS_B, TOP))
    routing_expert_weight = jnp.clip(0.2 + 0.8 * jax.random.uniform(part_splits[10], (TOKENS_B, TOP), jnp.float32) ** block_levels(part_splits[10], (TOKENS_B, TOP), ((0, 16),), -0.2, 0.2), 0.2, 1.0)
    expert_gate_matrix = bell_draw(seeds[11], (EXPERTS, D, FFE), D ** -0.5, 0.125, ((0, 4), (2, 4)))
    expert_up_matrix = bell_draw(seeds[12], (EXPERTS, D, FFE), D ** -0.5, 0.125, ((0, 4), (2, 4)))
    expert_down_matrix = bell_draw(seeds[13], (EXPERTS, FFE, D), FFE ** -0.5, 0.09375, ((0, 4), (1, 4)))
    return {"memory_query_rows": memory_query_rows, "memory_key_rows": memory_key_rows, "memory_value_rows": memory_value_rows, "input_gate_log": input_gate_log, "forget_gate_logits": forget_gate_logits, "forget_log_extra": forget_log_extra, "memory_output_weight": memory_output_weight, "second_batch_tokens": second_batch_tokens, "expert_norm_gain": expert_norm_gain, "routing_expert_index": routing_expert_index, "routing_expert_weight": routing_expert_weight, "expert_gate_matrix": expert_gate_matrix, "expert_up_matrix": expert_up_matrix, "expert_down_matrix": expert_down_matrix}


rms_eps = 1e-06
highest = lax.Precision.HIGHEST

def state_update(state_in, inputs, cumulative):
    memory, normer, stabilizer = state_in
    key_rows, values, in_gate, forget = inputs
    block_total = cumulative[:, -1]
    weights = block_total[:, None] - cumulative + in_gate
    new_stab = jnp.maximum(block_total + stabilizer, lax.optimization_barrier(jnp.max(weights, axis=-1)))
    scaled = jnp.exp(weights - new_stab[:, None])
    retained = jnp.exp(block_total + stabilizer - new_stab)
    weighted_keys = scaled[:, :, None] * key_rows
    memory = retained[:, None, None] * memory + jnp.einsum('hsd,hse->hde', weighted_keys, values, precision=highest)
    normer = retained[:, None] * normer + lax.optimization_barrier(jnp.sum(weighted_keys, axis=1))
    return (memory, normer, new_stab)

def block_step(state_in, inputs):
    memory, normer, stabilizer = state_in
    queries, key_rows, values, in_gate, forget = inputs
    length = queries.shape[1]
    causal = jnp.tril(jnp.ones((length, length), dtype=bool))
    cumulative = jnp.cumsum(forget, axis=-1)
    decays = jnp.where(causal, cumulative[:, :, None] - cumulative[:, None, :] + in_gate[:, None, :], -jnp.inf)
    carried_max = cumulative + stabilizer[:, None]
    row_max = jnp.maximum(lax.optimization_barrier(jnp.max(decays, axis=-1)), carried_max)
    scores = jnp.einsum('htd,hsd->hts', queries, key_rows, precision=highest) * jnp.exp(decays - row_max[:, :, None])
    carried = jnp.exp(carried_max - row_max)
    numerator = carried[:, :, None] * jnp.einsum('htd,hde->hte', queries, memory, precision=highest) + jnp.einsum('hts,hse->hte', scores, values, precision=highest)
    denominator = carried * jnp.einsum('htd,hd->ht', queries, normer, precision=highest) + lax.optimization_barrier(jnp.sum(scores, axis=-1))
    output = numerator / jnp.maximum(jnp.abs(denominator), jnp.exp(-row_max))[:, :, None]
    new_state = state_update(state_in, (key_rows, values, in_gate, forget), cumulative)
    return (new_state, output)

def split_blocks(row_block, heads):
    count = row_block.shape[0] // BLOCK
    return row_block.astype(jnp.float32).reshape(count, BLOCK, heads, -1).transpose(0, 2, 1, 3)

def gate_blocks(gate_rows):
    heads = gate_rows.shape[0]
    return gate_rows.reshape(heads, -1, BLOCK).transpose(1, 0, 2)

def expert_ffn(row_block, gate_weight, up_weight, down_weight):
    gate_act = jnp.dot(row_block, gate_weight, preferred_element_type=jnp.float32)
    up_act = jnp.dot(row_block, up_weight, preferred_element_type=jnp.float32)
    hidden = (jax.nn.silu(gate_act) * up_act).astype(jnp.bfloat16)
    group_width = FFE // N_TP
    running = jnp.zeros((row_block.shape[0], D), jnp.float32)
    for group in range(N_TP):
        part_rows = hidden[:, group * group_width:(group + 1) * group_width]
        part_down = down_weight[group * group_width:(group + 1) * group_width]
        partial_out = jnp.dot(part_rows, part_down, preferred_element_type=jnp.float32).astype(jnp.bfloat16)
        running = running + partial_out.astype(jnp.float32)
    return running.astype(jnp.bfloat16)

def reference(memory_query_rows, memory_key_rows, memory_value_rows, input_gate_log, forget_gate_logits, forget_log_extra, memory_output_weight, second_batch_tokens, expert_norm_gain, routing_expert_index, routing_expert_weight, expert_gate_matrix, expert_up_matrix, expert_down_matrix):
    queries = split_blocks(memory_query_rows, HM)
    key_rows = split_blocks(memory_key_rows, HM) * DH ** (-0.5)
    values = split_blocks(memory_value_rows, HM)
    forget_log_value = jax.nn.log_sigmoid(forget_gate_logits) + forget_log_extra
    start_state = (jnp.zeros((HM, DH, DH), jnp.float32), jnp.zeros((HM, DH), jnp.float32), jnp.zeros((HM,), jnp.float32))
    _, outputs = lax.scan(block_step, start_state, (queries, key_rows, values, gate_blocks(input_gate_log), gate_blocks(forget_log_value)))
    memory_rows = outputs.transpose(0, 2, 1, 3).reshape(SEQ_LEN, HM * DH).astype(jnp.bfloat16)
    mixed_out = jnp.dot(memory_rows, memory_output_weight, preferred_element_type=jnp.float32).astype(jnp.bfloat16)
    tokens_f = second_batch_tokens.astype(jnp.float32)
    normed = (tokens_f * lax.rsqrt(lax.optimization_barrier(jnp.mean(tokens_f * tokens_f, axis=1, keepdims=True)) + rms_eps) * expert_norm_gain).astype(jnp.bfloat16)
    devices = TOKENS_B // TOK_B_DEV
    flat_ids = routing_expert_index.reshape(devices, TOK_B_DEV * TOP)
    onehot = (flat_ids[:, :, None] == jnp.arange(EXPERTS, dtype=jnp.int32)[None, None, :]).astype(jnp.int32)
    route_ranks = lax.optimization_barrier(jnp.sum((jnp.cumsum(onehot, axis=1) - 1) * onehot, axis=2))
    owner = jnp.arange(devices, dtype=jnp.int32)[:, None]
    slot_ids = (flat_ids * (devices * CAP) + owner * CAP + route_ranks).reshape(-1).astype(jnp.int32)
    token_ids = jnp.repeat(jnp.arange(TOKENS_B, dtype=jnp.int32), TOP)
    slot_table = jnp.full((EXPERTS * devices * CAP,), TOKENS_B, jnp.int32).at[slot_ids].set(token_ids)
    padded = jnp.concatenate([normed, jnp.zeros((1, D), jnp.bfloat16)], axis=0)

    def one_expert(inputs):
        index_rows, gate_weight, up_weight, down_weight = inputs
        return expert_ffn(padded[index_rows], gate_weight, up_weight, down_weight)
    results = lax.map(one_expert, (slot_table.reshape(EXPERTS, devices * CAP), expert_gate_matrix, expert_up_matrix, expert_down_matrix))
    picked = results.reshape(-1, D)[slot_ids].astype(jnp.float32).reshape(TOKENS_B, TOP, D)
    expert_out = lax.optimization_barrier(jnp.sum(picked * routing_expert_weight[:, :, None], axis=1)).astype(jnp.bfloat16)
    return (mixed_out, expert_out)
```

```python
import functools

import jax
import jax.numpy as jnp
from jax import lax
from jax.experimental import pallas as pl
from jax.experimental.pallas import tpu as pltpu
from jax.sharding import PartitionSpec as P

DH = 128
TOP = 2
BLOCK = 128


neg_big = -1e30
rms_eps = 1e-06
highest = lax.Precision.HIGHEST


MESH = pl.DeviceIdType.MESH
LANES = 128


def expert_kernel(
    ep,
    tp,
    cap,
    out_ref,
    state_ref,
    gate_hbm,
    up_hbm,
    down_hbm,
    ret_ref,
    states_ref,
    gate_up,
    down,
    rows,
    hidden,
    part,
    near_part,
    pair_sum,
    far_part,
    result,
    w_sem,
    own_sem,
    st_sem,
    z_sem,
    far_sem,
    near_sem,
    relay_sem,
    np_sem,
    fp_sem,
    r_sem,
):
    e = lax.axis_index("ep")
    t = lax.axis_index("tp")
    side, core = t // 2, t % 2
    near = side * 2 + (1 - core)
    far = (1 - side) * 2 + core
    tiles = gate_up.shape[0]
    width = rows.shape[2]

    def place(side_at, core_at):
        return pl.ds(pl.multiple_of((core_at * 2 + side_at) * cap, cap), cap)

    mine = place(side, core)
    theirs = place(1 - side, core)

    def remote(src, dst, sems, k, target):
        return pltpu.make_async_remote_copy(
            src_ref=src,
            dst_ref=dst,
            send_sem=sems.at[0, k],
            recv_sem=sems.at[1, k],
            device_id=target,
            device_id_type=MESH,
        )

    def ahead(k):
        return {"ep": lax.rem(e + k, ep)}

    def behind(k):
        return {"ep": lax.rem(e + ep - k, ep)}

    def weight_copies(i):
        cols = pl.ds(pl.multiple_of(i * LANES, LANES), LANES)
        return (
            pltpu.make_async_copy(
                gate_hbm.at[0, :, cols], gate_up.at[i, :, pl.ds(0, LANES)], w_sem.at[0, i]
            ),
            pltpu.make_async_copy(
                up_hbm.at[0, :, cols], gate_up.at[i, :, pl.ds(LANES, LANES)], w_sem.at[1, i]
            ),
        )

    down_copy = pltpu.make_async_copy(down_hbm.at[0], down, own_sem.at[1])
    own_copy = pltpu.make_async_copy(out_ref.at[0], rows.at[0, mine], own_sem.at[0])

    def z_copy(k):
        return remote(out_ref.at[k], rows.at[k, mine], z_sem, k, ahead(k))

    def state_copy(k):
        return remote(state_ref, states_ref.at[k], st_sem, k, ahead(k))

    def far_copy(k):
        return remote(rows.at[k, mine], rows.at[k, mine], far_sem, k, {"tp": far})

    def near_copy(k):
        return remote(rows.at[k, mine], rows.at[k, mine], near_sem, k, {"tp": near})

    def relay_copy(k):
        return remote(rows.at[k, theirs], rows.at[k, theirs], relay_sem, k, {"tp": near})

    def near_part_copy(k):
        span = pl.ds(pl.multiple_of((1 - core) * 2 * cap, 2 * cap), 2 * cap)
        return remote(part.at[k, span], near_part.at[k], np_sem, k, {"tp": near})

    def far_part_copy(k):
        return remote(pair_sum.at[k], far_part.at[k], fp_sem, k, {"tp": far})

    def return_copy(k):
        return remote(result.at[k], ret_ref.at[k], r_sem, k, behind(k))

    barrier = pltpu.get_barrier_semaphore()

    @pl.loop(1, ep)
    def _(k):
        pl.semaphore_signal(barrier, inc=1, device_id=ahead(k), device_id_type=MESH)

    for target in (near, far):
        pl.semaphore_signal(barrier, inc=1, device_id={"tp": target}, device_id_type=MESH)
    own_copy.start()
    pl.semaphore_wait(barrier, ep + 1)

    @pl.loop(1, ep)
    def _(k):
        @pl.when(e + k < ep)
        def _():
            state_copy(k).start()

    @pl.loop(1, ep)
    def _(k):
        z_copy(k).start()

    own_copy.wait()
    far_copy(0).start()
    near_copy(0).start()

    @pl.loop(0, tiles)
    def _(i):
        for copy in weight_copies(i):
            copy.start()

    down_copy.start()

    def feed_forward(k):
        @pl.loop(0, tiles)
        def _(i):
            both = jnp.dot(rows[k], gate_up[i], preferred_element_type=jnp.float32)
            act, up_act = both[:, :LANES], both[:, LANES:]
            hidden[:, pl.ds(pl.multiple_of(i * LANES, LANES), LANES)] = (
                jax.nn.silu(act) * up_act
            ).astype(jnp.bfloat16)

        @pl.when(k == 0)
        def _():
            down_copy.wait()

        @pl.loop(0, width // 256)
        def _(i):
            cols = pl.ds(pl.multiple_of(i * 256, 256), 256)
            part[k, :, cols] = jnp.dot(
                hidden[...], down[:, cols], preferred_element_type=jnp.float32
            ).astype(jnp.bfloat16)

    def pair_stage(k):
        near_part_copy(k).wait_recv()
        other = pl.ds(pl.multiple_of((1 - side) * cap, cap), cap)
        pair_sum[k] = (
            part[k, theirs].astype(jnp.float32) + near_part[k, other].astype(jnp.float32)
        ).astype(jnp.bfloat16)
        far_part_copy(k).start()

    def final_stage(k):
        far_part_copy(k).wait_recv()
        own = pl.ds(pl.multiple_of(side * cap, cap), cap)
        total = (
            part[k, mine].astype(jnp.float32)
            + near_part[k, own].astype(jnp.float32)
            + far_part[k].astype(jnp.float32)
        ).astype(jnp.bfloat16)

        @pl.when(k == 0)
        def _():
            ret_ref[k] = total

        @pl.when(k > 0)
        def _():
            result[k] = total
            return_copy(k).start()

    @pl.loop(0, ep + 2)
    def _(k):
        @pl.when(k + 1 < ep)
        def _():
            z_copy(k + 1).wait_recv()
            far_copy(k + 1).start()
            near_copy(k + 1).start()

        @pl.when(k < ep)
        def _():
            far_copy(k).wait_recv()
            relay_copy(k).start()

        @pl.when((k >= 1) & (k <= ep))
        def _():
            pair_stage(k - 1)

        @pl.when(k >= 2)
        def _():
            final_stage(k - 2)

        @pl.when(k == 0)
        def _():
            @pl.loop(0, tiles)
            def _(i):
                for copy in weight_copies(i):
                    copy.wait()

        @pl.when(k < ep)
        def _():
            near_copy(k).wait_recv()
            relay_copy(k).wait_recv()
            feed_forward(k)
            near_part_copy(k).start()

    @pl.loop(0, ep)
    def _(k):
        far_copy(k).wait_send()
        near_copy(k).wait_send()
        relay_copy(k).wait_send()
        near_part_copy(k).wait_send()
        far_part_copy(k).wait_send()

    @pl.loop(1, ep)
    def _(k):
        z_copy(k).wait_send()

        @pl.when(e + k < ep)
        def _():
            state_copy(k).wait_send()

        @pl.when(e >= k)
        def _():
            state_copy(k).wait_recv()

        return_copy(k).wait()


def expert_exchange(outgoing, state, gate, up, down):
    ep, tp = lax.axis_size("ep"), lax.axis_size("tp")
    _, cap, width = outgoing.shape
    part_hidden = gate.shape[2]
    tiles = part_hidden // LANES
    bf16 = jnp.bfloat16
    vmem = pl.BlockSpec(memory_space=pltpu.VMEM)
    hbm = pl.BlockSpec(memory_space=pl.ANY)
    pair = pltpu.SemaphoreType.DMA((2, ep))
    rows = ep * tp * cap
    return pl.pallas_call(
        functools.partial(expert_kernel, ep, tp, cap),
        out_shape=(
            jax.ShapeDtypeStruct(outgoing.shape, bf16),
            jax.ShapeDtypeStruct((ep,) + state.shape, jnp.float32),
        ),
        in_specs=[vmem, vmem, hbm, hbm, hbm],
        out_specs=(vmem, hbm),
        scratch_shapes=[
            pltpu.VMEM((tiles, width, 2 * LANES), bf16),
            pltpu.VMEM((part_hidden, width), bf16),
            pltpu.VMEM((ep, tp * cap, width), bf16),
            pltpu.VMEM((tp * cap, part_hidden), bf16),
            pltpu.VMEM((ep, tp * cap, width), bf16),
            pltpu.VMEM((ep, 2 * cap, width), bf16),
            pltpu.VMEM((ep, cap, width), bf16),
            pltpu.VMEM((ep, cap, width), bf16),
            pltpu.VMEM((ep, cap, width), bf16),
            pltpu.SemaphoreType.DMA((2, tiles)),
            pltpu.SemaphoreType.DMA((2,)),
        ]
        + [pair] * 8,
        compiler_params=pltpu.CompilerParams(
            collective_id=0, has_side_effects=True, vmem_limit_bytes=66000000
        ),
        cost_estimate=pl.CostEstimate(
            flops=6 * rows * width * part_hidden, bytes_accessed=6 * width * part_hidden,
            transcendentals=rows * part_hidden,
        ),
    )(outgoing, state, gate, up, down)


def pack_state(memory, normer, stabilizer, totals):
    heads = memory.shape[0]
    extra = jnp.concatenate(
        [
            normer[:, None, :],
            jnp.broadcast_to(stabilizer[:, None, None], (heads, 1, DH)),
            jnp.broadcast_to(totals[:, None, None], (heads, 1, DH)),
            jnp.zeros((heads, 5, DH), jnp.float32),
        ],
        axis=1,
    )
    return jnp.concatenate([memory, extra], axis=1)


def entering_state(states):
    place = lax.axis_index("ep")
    count = states.shape[0]
    turn = jnp.arange(count)
    valid = (turn >= 1) & (turn <= place)
    memory = jnp.where(valid[:, None, None, None], states[:, :, :DH], 0.0)
    normer = jnp.where(valid[:, None, None], states[:, :, DH], 0.0)
    stab = jnp.where(valid[:, None], states[:, :, DH + 1, 0], neg_big)
    totals = jnp.where(valid[:, None], states[:, :, DH + 2, 0], 0.0)
    nearer = turn[None, :] < turn[:, None]
    later = jnp.sum(jnp.where(nearer[:, :, None], totals[None], 0.0), axis=1)
    level = jnp.where(valid[:, None], stab + later, neg_big)
    stab_in = jnp.maximum(jnp.sum(totals, axis=0), jnp.max(level, axis=0))
    scale = jnp.where(valid[:, None], jnp.exp(level - stab_in[None]), 0.0)
    memory = jnp.sum(scale[:, :, None, None] * memory, axis=0)
    normer = jnp.sum(scale[:, :, None] * normer, axis=0)
    return memory, normer, stab_in


def state_update(state_in, inputs, cumulative):
    memory, normer, stabilizer = state_in
    key_rows, values, in_gate, forget = inputs
    block_total = cumulative[:, -1]
    weights = block_total[:, None] - cumulative + in_gate
    new_stab = jnp.maximum(block_total + stabilizer, jnp.max(weights, axis=-1))
    scaled = jnp.exp(weights - new_stab[:, None])
    retained = jnp.exp(block_total + stabilizer - new_stab)
    weighted_keys = scaled[:, :, None] * key_rows
    memory = retained[:, None, None] * memory + jnp.einsum(
        "hsd,hse->hde", weighted_keys, values, precision=highest
    )
    normer = retained[:, None] * normer + jnp.sum(weighted_keys, axis=1)
    return (memory, normer, new_stab)


def state_only(state_in, inputs):
    cumulative = jnp.cumsum(inputs[3], axis=-1)
    return (state_update(state_in, inputs, cumulative), None)


def block_step(state_in, inputs):
    memory, normer, stabilizer = state_in
    queries, key_rows, values, in_gate, forget = inputs
    length = queries.shape[1]
    causal = jnp.tril(jnp.ones((length, length), dtype=bool))
    cumulative = jnp.cumsum(forget, axis=-1)
    decays = jnp.where(
        causal, cumulative[:, :, None] - cumulative[:, None, :] + in_gate[:, None, :], -jnp.inf
    )
    carried_max = cumulative + stabilizer[:, None]
    row_max = jnp.maximum(jnp.max(decays, axis=-1), carried_max)
    scores = jnp.einsum("htd,hsd->hts", queries, key_rows, precision=highest) * jnp.exp(
        decays - row_max[:, :, None]
    )
    carried = jnp.exp(carried_max - row_max)
    numerator = carried[:, :, None] * jnp.einsum(
        "htd,hde->hte", queries, memory, precision=highest
    ) + jnp.einsum("hts,hse->hte", scores, values, precision=highest)
    denominator = carried * jnp.einsum("htd,hd->ht", queries, normer, precision=highest) + jnp.sum(
        scores, axis=-1
    )
    output = numerator / jnp.maximum(jnp.abs(denominator), jnp.exp(-row_max))[:, :, None]
    new_state = state_update(state_in, (key_rows, values, in_gate, forget), cumulative)
    return (new_state, output)


def split_blocks(row_block, heads):
    count = row_block.shape[0] // BLOCK
    return row_block.astype(jnp.float32).reshape(count, BLOCK, heads, -1).transpose(0, 2, 1, 3)


def gate_blocks(gate_rows):
    heads = gate_rows.shape[0]
    return gate_rows.reshape(heads, -1, BLOCK).transpose(1, 0, 2)


def route_slots(routing_expert_index, experts, stride):
    flat_ids = routing_expert_index.reshape(-1)
    onehot = (flat_ids[:, None] == jnp.arange(experts, dtype=jnp.int32)[None, :]).astype(jnp.int32)
    route_ranks = jnp.sum((jnp.cumsum(onehot, axis=0) - 1) * onehot, axis=1)
    turn = lax.rem(flat_ids + experts - lax.axis_index("ep"), experts)
    return (turn * stride + route_ranks).reshape(routing_expert_index.shape)


def on_device(
    memory_query_rows,
    memory_key_rows,
    memory_value_rows,
    input_gate_log,
    forget_gate_logits,
    forget_log_extra,
    memory_output_weight,
    second_batch_tokens,
    expert_norm_gain,
    routing_expert_index,
    routing_expert_weight,
    expert_gate_matrix,
    expert_up_matrix,
    expert_down_matrix,
):
    heads_local = input_gate_log.shape[0]
    positions = input_gate_log.shape[1]
    queries = split_blocks(memory_query_rows, heads_local)
    key_rows = split_blocks(memory_key_rows, heads_local) * DH ** (-0.5)
    values = split_blocks(memory_value_rows, heads_local)
    in_gate = gate_blocks(input_gate_log)
    forget_log_value = jax.nn.log_sigmoid(forget_gate_logits) + forget_log_extra
    forget = gate_blocks(forget_log_value)
    zero_memory = jnp.zeros((heads_local, DH, DH), jnp.float32)
    zero_normer = jnp.zeros((heads_local, DH), jnp.float32)
    low_stab = jnp.full((heads_local,), neg_big, jnp.float32)
    local_state, _ = lax.scan(
        state_only, (zero_memory, zero_normer, low_stab), (key_rows, values, in_gate, forget)
    )
    totals = jnp.sum(forget_log_value, axis=1)
    tok_rows = second_batch_tokens.shape[0]
    experts = lax.axis_size("ep")
    capacity = max(2, 5 * tok_rows * TOP // (4 * experts))
    stride = -(-capacity // 16) * 16
    slots_dev = experts * stride
    tokens_f = second_batch_tokens.astype(jnp.float32)
    normed = (
        tokens_f
        * lax.rsqrt(jnp.mean(tokens_f * tokens_f, axis=1, keepdims=True) + rms_eps)
        * expert_norm_gain
    ).astype(jnp.bfloat16)
    slot_ids = route_slots(routing_expert_index, experts, stride)
    slot_table = jnp.arange(slots_dev, dtype=jnp.int32)
    placing = jnp.zeros((slots_dev, tok_rows), jnp.bfloat16)
    for column in range(TOP):
        placing = placing + (slot_table[:, None] == slot_ids[None, :, column]).astype(jnp.bfloat16)
    outgoing = jnp.dot(placing, normed, preferred_element_type=jnp.float32).astype(jnp.bfloat16)
    returned, states = expert_exchange(
        outgoing.reshape(experts, stride, -1),
        pack_state(*local_state, totals),
        expert_gate_matrix,
        expert_up_matrix,
        expert_down_matrix,
    )
    incoming = entering_state(states)
    _, outputs = lax.scan(block_step, incoming, (queries, key_rows, values, in_gate, forget))
    memory_rows = outputs.transpose(0, 2, 1, 3).reshape(positions, -1).astype(jnp.bfloat16)
    mixed = jnp.dot(
        lax.all_gather(memory_rows, "tp", axis=1, tiled=True),
        memory_output_weight,
        preferred_element_type=jnp.float32,
    )
    mixed_out = mixed.astype(jnp.bfloat16)
    choosing = jnp.zeros((tok_rows, slots_dev), jnp.float32)
    for column in range(TOP):
        choosing = choosing + jnp.where(
            slot_table[None, :] == slot_ids[:, column : column + 1],
            routing_expert_weight[:, column : column + 1],
            0.0,
        )
    expert_out = jnp.dot(
        choosing, returned.reshape(slots_dev, -1).astype(jnp.float32), precision=highest
    ).astype(jnp.bfloat16)
    return (mixed_out, expert_out)


def solution(mesh):
    placed = (
        P(("grp", "ep"), "tp"),
        P(("grp", "ep"), "tp"),
        P(("grp", "ep"), "tp"),
        P("tp", ("grp", "ep")),
        P("tp", ("grp", "ep")),
        P("tp", ("grp", "ep")),
        P(None, "tp"),
        P(("grp", "ep", "tp"), None),
        P(),
        P(("grp", "ep", "tp"), None),
        P(("grp", "ep", "tp"), None),
        P("ep", None, "tp"),
        P("ep", None, "tp"),
        P("ep", "tp", None),
    )
    return jax.shard_map(
        on_device,
        mesh=mesh,
        in_specs=placed,
        out_specs=(P(("grp", "ep"), "tp"), P(("grp", "ep", "tp"), None)),
        check_vma=False,
    )
```

```python
import functools

import jax
import jax.numpy as jnp
from jax import lax
from jax.experimental import pallas as pl
from jax.experimental.pallas import tpu as pltpu
from jax.sharding import PartitionSpec as P

DH = 128
TOP = 2
BLOCK = 128


neg_big = -1e30
rms_eps = 1e-06
highest = lax.Precision.HIGHEST


MESH = pl.DeviceIdType.MESH
LANES = 128


def expert_kernel(
    ep,
    tp,
    cap,
    out_ref,
    query_ref,
    key_ref,
    value_ref,
    in_gate_ref,
    logit_ref,
    extra_ref,
    mix_hbm,
    gate_hbm,
    up_hbm,
    down_hbm,
    ret_ref,
    mixed_ref,
    gate_up,
    down,
    rows,
    hidden,
    part,
    near_part,
    pair_sum,
    far_part,
    result,
    local_state,
    state_in,
    state_out,
    memory,
    mix,
    w_sem,
    own_sem,
    st_sem,
    z_sem,
    far_sem,
    near_sem,
    relay_sem,
    np_sem,
    fp_sem,
    r_sem,
    m_sem,
):
    e = lax.axis_index("ep")
    t = lax.axis_index("tp")
    side, core = t // 2, t % 2
    near = side * 2 + (1 - core)
    far = (1 - side) * 2 + core
    across = (1 - side) * 2 + (1 - core)
    heads = in_gate_ref.shape[0]
    length = in_gate_ref.shape[1]
    tiles = gate_up.shape[0]
    width = rows.shape[2]

    def place(side_at, core_at):
        return pl.ds(pl.multiple_of((core_at * 2 + side_at) * cap, cap), cap)

    mine = place(side, core)
    theirs = place(1 - side, core)

    def remote(src, dst, sems, k, target):
        return pltpu.make_async_remote_copy(
            src_ref=src,
            dst_ref=dst,
            send_sem=sems.at[0, k],
            recv_sem=sems.at[1, k],
            device_id=target,
            device_id_type=MESH,
        )

    def ahead(k):
        return {"ep": lax.rem(e + k, ep)}

    def behind(k):
        return {"ep": lax.rem(e + ep - k, ep)}

    def weight_copies(i):
        cols = pl.ds(pl.multiple_of(i * LANES, LANES), LANES)
        return (
            pltpu.make_async_copy(
                gate_hbm.at[0, :, cols], gate_up.at[i, :, pl.ds(0, LANES)], w_sem.at[0, i]
            ),
            pltpu.make_async_copy(
                up_hbm.at[0, :, cols], gate_up.at[i, :, pl.ds(LANES, LANES)], w_sem.at[1, i]
            ),
        )

    down_copy = pltpu.make_async_copy(down_hbm.at[0], down, own_sem.at[1])
    own_copy = pltpu.make_async_copy(out_ref.at[0], rows.at[0, mine], own_sem.at[0])

    def z_copy(k):
        return remote(out_ref.at[k], rows.at[k, mine], z_sem, k, ahead(k))

    state_copy = remote(state_out, state_in, st_sem, 0, ahead(1))
    mix_copy = pltpu.make_async_copy(mix_hbm, mix, own_sem.at[2])

    def memory_copy(i):
        span = memory.at[t]
        return remote(span, span, m_sem, i, {"tp": (near, far, across)[i]})

    def gates(h):
        logits = logit_ref[h : h + 1, :]
        forget = (
            jnp.minimum(logits, 0.0) - jnp.log1p(jnp.exp(-jnp.abs(logits)))
        ) + extra_ref[h : h + 1, :]
        at_row = lax.broadcasted_iota(jnp.int32, (length, length), 0)
        at_col = lax.broadcasted_iota(jnp.int32, (length, length), 1)
        diagonal = at_row == at_col
        in_row = in_gate_ref[h : h + 1, :]
        in_col = jnp.sum(jnp.where(diagonal, in_row, 0.0), axis=1, keepdims=True)
        sum_col = jnp.sum(jnp.where(at_col <= at_row, forget, 0.0), axis=1, keepdims=True)
        sum_row = jnp.sum(jnp.where(diagonal, sum_col, 0.0), axis=0, keepdims=True)
        total = jnp.sum(forget, axis=1, keepdims=True)
        return in_row, in_col, sum_row, sum_col, total, at_col <= at_row

    def head(ref, h):
        return ref[:, h * DH : (h + 1) * DH].astype(jnp.float32)

    def local_part():
        for h in range(heads):
            _, in_col, _, sum_col, total, _ = gates(h)
            weights = total - sum_col + in_col
            stab = jnp.max(weights, axis=0, keepdims=True)
            weighted = jnp.exp(weights - stab) * (head(key_ref, h) * DH ** (-0.5))
            local_state[h, 0:DH, :] = jnp.dot(
                weighted.T, head(value_ref, h), precision=highest,
                preferred_element_type=jnp.float32,
            )
            local_state[h, DH : DH + 1, :] = jnp.sum(weighted, axis=0, keepdims=True)
            local_state[h, DH + 1 : DH + 2, :] = jnp.broadcast_to(stab, (1, DH))
            local_state[h, DH + 2 : DH + 3, :] = jnp.broadcast_to(total, (1, DH))

    def pass_state():
        for h in range(heads):
            total = local_state[h, DH + 2 : DH + 3, :]
            stab_own = local_state[h, DH + 1 : DH + 2, :]
            carried = total + state_in[h, DH + 1 : DH + 2, :]
            stab = jnp.maximum(carried, stab_own)
            old, new = jnp.exp(carried - stab), jnp.exp(stab_own - stab)
            state_out[h, 0 : DH + 1, :] = (
                old * state_in[h, 0 : DH + 1, :] + new * local_state[h, 0 : DH + 1, :]
            )
            state_out[h, DH + 1 : DH + 2, :] = stab
        state_copy.start()

    def memory_part():
        for h in range(heads):
            in_row, _, sum_row, sum_col, _, causal = gates(h)
            decays = jnp.where(causal, sum_col - sum_row + in_row, -jnp.inf)
            carried_max = sum_col + state_in[h, DH + 1 : DH + 2, 0:1]
            row_max = jnp.maximum(jnp.max(decays, axis=1, keepdims=True), carried_max)
            queries = head(query_ref, h)
            keys = head(key_ref, h) * DH ** (-0.5)
            scores = jnp.dot(
                queries, keys.T, precision=highest, preferred_element_type=jnp.float32
            ) * jnp.exp(decays - row_max)
            carried = jnp.exp(carried_max - row_max)
            numerator = carried * jnp.dot(
                queries, state_in[h, 0:DH, :], precision=highest,
                preferred_element_type=jnp.float32,
            ) + jnp.dot(
                scores, head(value_ref, h), precision=highest,
                preferred_element_type=jnp.float32,
            )
            denominator = carried * jnp.sum(
                queries * state_in[h, DH : DH + 1, :], axis=1, keepdims=True
            ) + jnp.sum(scores, axis=1, keepdims=True)
            memory[t, :, h * DH : (h + 1) * DH] = (
                numerator / jnp.maximum(jnp.abs(denominator), jnp.exp(-row_max))
            ).astype(jnp.bfloat16)
        for i in range(3):
            memory_copy(i).start()

    def mix_part():
        mix_copy.wait()
        for i in range(3):
            memory_copy(i).wait_recv()
        total = jnp.zeros(mixed_ref.shape, jnp.float32)
        for i in range(tp):
            total = total + jnp.dot(
                memory[i], mix[i * heads * DH : (i + 1) * heads * DH, :],
                preferred_element_type=jnp.float32,
            )
        mixed_ref[...] = total.astype(jnp.bfloat16)

    def far_copy(k):
        return remote(rows.at[k, mine], rows.at[k, mine], far_sem, k, {"tp": far})

    def near_copy(k):
        return remote(rows.at[k, mine], rows.at[k, mine], near_sem, k, {"tp": near})

    def relay_copy(k):
        return remote(rows.at[k, theirs], rows.at[k, theirs], relay_sem, k, {"tp": near})

    def near_part_copy(k):
        span = pl.ds(pl.multiple_of((1 - core) * 2 * cap, 2 * cap), 2 * cap)
        return remote(part.at[k, span], near_part.at[k], np_sem, k, {"tp": near})

    def far_part_copy(k):
        return remote(pair_sum.at[k], far_part.at[k], fp_sem, k, {"tp": far})

    def return_copy(k):
        return remote(result.at[k], ret_ref.at[k], r_sem, k, behind(k))

    barrier = pltpu.get_barrier_semaphore()

    @pl.loop(1, ep)
    def _(k):
        pl.semaphore_signal(barrier, inc=1, device_id=ahead(k), device_id_type=MESH)

    for target in (near, far, across):
        pl.semaphore_signal(barrier, inc=1, device_id={"tp": target}, device_id_type=MESH)
    own_copy.start()
    pl.semaphore_wait(barrier, ep + 2)

    @pl.when(ep > 1)
    def _():
        z_copy(1).start()

    own_copy.wait()
    far_copy(0).start()
    near_copy(0).start()

    @pl.loop(0, tiles)
    def _(i):
        for copy in weight_copies(i):
            copy.start()

    down_copy.start()
    mix_copy.start()
    local_part()

    @pl.when(e == 0)
    def _():
        state_in[...] = jnp.zeros_like(state_in)
        if ep > 1:
            pass_state()

    def feed_forward(k):
        @pl.loop(0, tiles)
        def _(i):
            both = jnp.dot(rows[k], gate_up[i], preferred_element_type=jnp.float32)
            act, up_act = both[:, :LANES], both[:, LANES:]
            hidden[:, pl.ds(pl.multiple_of(i * LANES, LANES), LANES)] = (
                jax.nn.silu(act) * up_act
            ).astype(jnp.bfloat16)

        @pl.when(k == 0)
        def _():
            down_copy.wait()

        @pl.loop(0, width // 256)
        def _(i):
            cols = pl.ds(pl.multiple_of(i * 256, 256), 256)
            part[k, :, cols] = jnp.dot(
                hidden[...], down[:, cols], preferred_element_type=jnp.float32
            ).astype(jnp.bfloat16)

    def pair_stage(k):
        near_part_copy(k).wait_recv()
        other = pl.ds(pl.multiple_of((1 - side) * cap, cap), cap)
        pair_sum[k] = (
            part[k, theirs].astype(jnp.float32) + near_part[k, other].astype(jnp.float32)
        ).astype(jnp.bfloat16)
        far_part_copy(k).start()

    def final_stage(k):
        far_part_copy(k).wait_recv()
        own = pl.ds(pl.multiple_of(side * cap, cap), cap)
        total = (
            part[k, mine].astype(jnp.float32)
            + near_part[k, own].astype(jnp.float32)
            + far_part[k].astype(jnp.float32)
        ).astype(jnp.bfloat16)

        @pl.when(k == 0)
        def _():
            ret_ref[k] = total

        @pl.when(k > 0)
        def _():
            result[k] = total
            return_copy(k).start()

    @pl.loop(0, ep + 1)
    def _(k):
        @pl.when(k >= 1)
        def _():
            pair_stage(k - 1)

        @pl.when(k < ep)
        def _():
            far_copy(k).wait_recv()
            relay_copy(k).start()

        @pl.when(k + 1 < ep)
        def _():
            z_copy(k + 1).wait_recv()
            far_copy(k + 1).start()
            near_copy(k + 1).start()

        @pl.when(k + 2 < ep)
        def _():
            z_copy(k + 2).start()

        @pl.when(k == 0)
        def _():
            @pl.loop(0, tiles)
            def _(i):
                for copy in weight_copies(i):
                    copy.wait()

        @pl.when(k < ep)
        def _():
            near_copy(k).wait_recv()
            relay_copy(k).wait_recv()
            feed_forward(k)
            near_part_copy(k).start()

        @pl.when((k > 0) & (e == k))
        def _():
            state_copy.wait_recv()

            @pl.when(e + 1 < ep)
            def _():
                pass_state()

        @pl.when((k < ep) & (e == k))
        def _():
            memory_part()

        @pl.when(k >= 1)
        def _():
            final_stage(k - 1)

    mix_part()
    for i in range(3):
        memory_copy(i).wait_send()

    @pl.when(e + 1 < ep)
    def _():
        state_copy.wait_send()

    @pl.loop(0, ep)
    def _(k):
        far_copy(k).wait_send()
        near_copy(k).wait_send()
        relay_copy(k).wait_send()
        near_part_copy(k).wait_send()
        far_part_copy(k).wait_send()

    @pl.loop(1, ep)
    def _(k):
        z_copy(k).wait_send()

        return_copy(k).wait()


def expert_exchange(outgoing, memory_args, mix_weight, gate, up, down):
    ep, tp = lax.axis_size("ep"), lax.axis_size("tp")
    _, cap, width = outgoing.shape
    part_hidden = gate.shape[2]
    tiles = part_hidden // LANES
    bf16 = jnp.bfloat16
    vmem = pl.BlockSpec(memory_space=pltpu.VMEM)
    hbm = pl.BlockSpec(memory_space=pl.ANY)
    pair = pltpu.SemaphoreType.DMA((2, ep))
    rows = ep * tp * cap
    positions = memory_args[0].shape[0]
    heads = memory_args[3].shape[0]
    state = pltpu.VMEM((heads, DH + 8, DH), jnp.float32)
    return pl.pallas_call(
        functools.partial(expert_kernel, ep, tp, cap),
        out_shape=(
            jax.ShapeDtypeStruct(outgoing.shape, bf16),
            jax.ShapeDtypeStruct((positions, mix_weight.shape[1]), bf16),
        ),
        in_specs=[vmem] * 7 + [hbm] * 4,
        out_specs=(vmem, vmem),
        scratch_shapes=[
            pltpu.VMEM((tiles, width, 2 * LANES), bf16),
            pltpu.VMEM((part_hidden, width), bf16),
            pltpu.VMEM((ep, tp * cap, width), bf16),
            pltpu.VMEM((tp * cap, part_hidden), bf16),
            pltpu.VMEM((ep, tp * cap, width), bf16),
            pltpu.VMEM((ep, 2 * cap, width), bf16),
            pltpu.VMEM((ep, cap, width), bf16),
            pltpu.VMEM((ep, cap, width), bf16),
            pltpu.VMEM((ep, cap, width), bf16),
            state,
            state,
            state,
            pltpu.VMEM((tp, positions, heads * DH), bf16),
            pltpu.VMEM(mix_weight.shape, bf16),
            pltpu.SemaphoreType.DMA((2, tiles)),
            pltpu.SemaphoreType.DMA((3,)),
        ]
        + [pair] * 8
        + [pltpu.SemaphoreType.DMA((2, 3))],
        compiler_params=pltpu.CompilerParams(
            collective_id=0, has_side_effects=True, vmem_limit_bytes=66000000
        ),
        cost_estimate=pl.CostEstimate(
            flops=6 * rows * width * part_hidden, bytes_accessed=6 * width * part_hidden,
            transcendentals=rows * part_hidden,
        ),
    )(outgoing, *memory_args, mix_weight, gate, up, down)


def route_slots(routing_expert_index, experts, stride):
    flat_ids = routing_expert_index.reshape(-1)
    onehot = (flat_ids[:, None] == jnp.arange(experts, dtype=jnp.int32)[None, :]).astype(jnp.int32)
    route_ranks = jnp.sum((jnp.cumsum(onehot, axis=0) - 1) * onehot, axis=1)
    turn = lax.rem(flat_ids + experts - lax.axis_index("ep"), experts)
    return (turn * stride + route_ranks).reshape(routing_expert_index.shape)


def on_device(
    memory_query_rows,
    memory_key_rows,
    memory_value_rows,
    input_gate_log,
    forget_gate_logits,
    forget_log_extra,
    memory_output_weight,
    second_batch_tokens,
    expert_norm_gain,
    routing_expert_index,
    routing_expert_weight,
    expert_gate_matrix,
    expert_up_matrix,
    expert_down_matrix,
):
    tok_rows = second_batch_tokens.shape[0]
    experts = lax.axis_size("ep")
    capacity = max(2, 5 * tok_rows * TOP // (4 * experts))
    stride = -(-capacity // 16) * 16
    slots_dev = experts * stride
    tokens_f = second_batch_tokens.astype(jnp.float32)
    normed = (
        tokens_f
        * lax.rsqrt(jnp.mean(tokens_f * tokens_f, axis=1, keepdims=True) + rms_eps)
        * expert_norm_gain
    ).astype(jnp.bfloat16)
    slot_ids = route_slots(routing_expert_index, experts, stride)
    slot_table = jnp.arange(slots_dev, dtype=jnp.int32)
    placing = jnp.zeros((slots_dev, tok_rows), jnp.bfloat16)
    for column in range(TOP):
        placing = placing + (slot_table[:, None] == slot_ids[None, :, column]).astype(jnp.bfloat16)
    outgoing = jnp.dot(placing, normed, preferred_element_type=jnp.float32).astype(jnp.bfloat16)
    returned, mixed_out = expert_exchange(
        outgoing.reshape(experts, stride, -1),
        (
            memory_query_rows,
            memory_key_rows,
            memory_value_rows,
            input_gate_log,
            forget_gate_logits,
            forget_log_extra,
        ),
        memory_output_weight,
        expert_gate_matrix,
        expert_up_matrix,
        expert_down_matrix,
    )
    choosing = jnp.zeros((tok_rows, slots_dev), jnp.float32)
    for column in range(TOP):
        choosing = choosing + jnp.where(
            slot_table[None, :] == slot_ids[:, column : column + 1],
            routing_expert_weight[:, column : column + 1],
            0.0,
        )
    expert_out = jnp.dot(
        choosing, returned.reshape(slots_dev, -1).astype(jnp.float32), precision=highest
    ).astype(jnp.bfloat16)
    return (mixed_out, expert_out)


def solution(mesh):
    placed = (
        P(("grp", "ep"), "tp"),
        P(("grp", "ep"), "tp"),
        P(("grp", "ep"), "tp"),
        P("tp", ("grp", "ep")),
        P("tp", ("grp", "ep")),
        P("tp", ("grp", "ep")),
        P(None, "tp"),
        P(("grp", "ep", "tp"), None),
        P(),
        P(("grp", "ep", "tp"), None),
        P(("grp", "ep", "tp"), None),
        P("ep", None, "tp"),
        P("ep", None, "tp"),
        P("ep", "tp", None),
    )
    return jax.shard_map(
        on_device,
        mesh=mesh,
        in_specs=placed,
        out_specs=(P(("grp", "ep"), "tp"), P(("grp", "ep", "tp"), None)),
        check_vma=False,
    )
```

```python
import functools

import jax
import jax.numpy as jnp
from jax import lax
from jax.experimental import pallas as pl
from jax.experimental.pallas import tpu as pltpu
from jax.sharding import PartitionSpec as P

DH = 128
TOP = 2
BLOCK = 128


neg_big = -1e30
rms_eps = 1e-06
highest = lax.Precision.HIGHEST


MESH = pl.DeviceIdType.MESH
LANES = 128


def expert_kernel(
    ep,
    tp,
    cap,
    out_ref,
    query_ref,
    key_ref,
    value_ref,
    in_gate_ref,
    logit_ref,
    extra_ref,
    mix_hbm,
    gate_hbm,
    up_hbm,
    down_hbm,
    ret_ref,
    mixed_ref,
    gate_up,
    down,
    rows,
    hidden,
    part,
    near_part,
    pair_sum,
    far_part,
    result,
    local_state,
    state_in,
    state_out,
    memory,
    mix,
    w_sem,
    own_sem,
    st_sem,
    z_sem,
    far_sem,
    near_sem,
    relay_sem,
    np_sem,
    fp_sem,
    r_sem,
    m_sem,
):
    e = lax.axis_index("ep")
    t = lax.axis_index("tp")
    side, core = t // 2, t % 2
    near = side * 2 + (1 - core)
    far = (1 - side) * 2 + core
    across = (1 - side) * 2 + (1 - core)
    heads = in_gate_ref.shape[0]
    length = in_gate_ref.shape[1]
    tiles = gate_up.shape[0]
    width = rows.shape[2]

    def place(side_at, core_at):
        return pl.ds(pl.multiple_of((core_at * 2 + side_at) * cap, cap), cap)

    mine = place(side, core)
    theirs = place(1 - side, core)

    def remote(src, dst, sems, k, target):
        return pltpu.make_async_remote_copy(
            src_ref=src,
            dst_ref=dst,
            send_sem=sems.at[0, k],
            recv_sem=sems.at[1, k],
            device_id=target,
            device_id_type=MESH,
        )

    def ahead(k):
        return {"ep": lax.rem(e + k, ep)}

    def behind(k):
        return {"ep": lax.rem(e + ep - k, ep)}

    def weight_copies(i):
        cols = pl.ds(pl.multiple_of(i * LANES, LANES), LANES)
        return (
            pltpu.make_async_copy(
                gate_hbm.at[0, :, cols], gate_up.at[i, :, pl.ds(0, LANES)], w_sem.at[0, i]
            ),
            pltpu.make_async_copy(
                up_hbm.at[0, :, cols], gate_up.at[i, :, pl.ds(LANES, LANES)], w_sem.at[1, i]
            ),
        )

    down_copy = pltpu.make_async_copy(down_hbm.at[0], down, own_sem.at[1])
    own_copy = pltpu.make_async_copy(out_ref.at[0], rows.at[0, mine], own_sem.at[0])

    def z_copy(k):
        return remote(out_ref.at[k], rows.at[k, mine], z_sem, k, ahead(k))

    state_copy = remote(state_out, state_in, st_sem, 0, ahead(1))
    mix_copy = pltpu.make_async_copy(mix_hbm, mix, own_sem.at[2])

    def memory_copy(i):
        span = memory.at[t]
        return remote(span, span, m_sem, i, {"tp": (near, far, across)[i]})

    def gates(h):
        logits = logit_ref[h : h + 1, :]
        forget = (
            jnp.minimum(logits, 0.0) - jnp.log1p(jnp.exp(-jnp.abs(logits)))
        ) + extra_ref[h : h + 1, :]
        at_row = lax.broadcasted_iota(jnp.int32, (length, length), 0)
        at_col = lax.broadcasted_iota(jnp.int32, (length, length), 1)
        diagonal = at_row == at_col
        in_row = in_gate_ref[h : h + 1, :]
        in_col = jnp.sum(jnp.where(diagonal, in_row, 0.0), axis=1, keepdims=True)
        sum_col = jnp.sum(jnp.where(at_col <= at_row, forget, 0.0), axis=1, keepdims=True)
        sum_row = jnp.sum(jnp.where(diagonal, sum_col, 0.0), axis=0, keepdims=True)
        total = jnp.sum(forget, axis=1, keepdims=True)
        return in_row, in_col, sum_row, sum_col, total, at_col <= at_row

    def head(ref, h):
        return ref[:, h * DH : (h + 1) * DH].astype(jnp.float32)

    def local_part():
        for h in range(heads):
            _, in_col, _, sum_col, total, _ = gates(h)
            weights = total - sum_col + in_col
            stab = jnp.max(weights, axis=0, keepdims=True)
            weighted = jnp.exp(weights - stab) * (head(key_ref, h) * DH ** (-0.5))
            local_state[h, 0:DH, :] = jnp.dot(
                weighted.T, head(value_ref, h), precision=highest,
                preferred_element_type=jnp.float32,
            )
            local_state[h, DH : DH + 1, :] = jnp.sum(weighted, axis=0, keepdims=True)
            local_state[h, DH + 1 : DH + 2, :] = jnp.broadcast_to(stab, (1, DH))
            local_state[h, DH + 2 : DH + 3, :] = jnp.broadcast_to(total, (1, DH))

    def pass_state():
        for h in range(heads):
            total = local_state[h, DH + 2 : DH + 3, :]
            stab_own = local_state[h, DH + 1 : DH + 2, :]
            carried = total + state_in[h, DH + 1 : DH + 2, :]
            stab = jnp.maximum(carried, stab_own)
            old, new = jnp.exp(carried - stab), jnp.exp(stab_own - stab)
            state_out[h, 0 : DH + 1, :] = (
                old * state_in[h, 0 : DH + 1, :] + new * local_state[h, 0 : DH + 1, :]
            )
            state_out[h, DH + 1 : DH + 2, :] = stab
        state_copy.start()

    def memory_part():
        for h in range(heads):
            in_row, _, sum_row, sum_col, _, causal = gates(h)
            decays = jnp.where(causal, sum_col - sum_row + in_row, -jnp.inf)
            carried_max = sum_col + state_in[h, DH + 1 : DH + 2, 0:1]
            row_max = jnp.maximum(jnp.max(decays, axis=1, keepdims=True), carried_max)
            queries = head(query_ref, h)
            keys = head(key_ref, h) * DH ** (-0.5)
            scores = jnp.dot(
                queries, keys.T, precision=highest, preferred_element_type=jnp.float32
            ) * jnp.exp(decays - row_max)
            carried = jnp.exp(carried_max - row_max)
            numerator = carried * jnp.dot(
                queries, state_in[h, 0:DH, :], precision=highest,
                preferred_element_type=jnp.float32,
            ) + jnp.dot(
                scores, head(value_ref, h), precision=highest,
                preferred_element_type=jnp.float32,
            )
            denominator = carried * jnp.sum(
                queries * state_in[h, DH : DH + 1, :], axis=1, keepdims=True
            ) + jnp.sum(scores, axis=1, keepdims=True)
            memory[t, :, h * DH : (h + 1) * DH] = (
                numerator / jnp.maximum(jnp.abs(denominator), jnp.exp(-row_max))
            ).astype(jnp.bfloat16)
        for i in range(3):
            memory_copy(i).start()

    def mix_part():
        mix_copy.wait()
        for i in range(3):
            memory_copy(i).wait_recv()
        total = jnp.zeros(mixed_ref.shape, jnp.float32)
        for i in range(tp):
            total = total + jnp.dot(
                memory[i], mix[i * heads * DH : (i + 1) * heads * DH, :],
                preferred_element_type=jnp.float32,
            )
        mixed_ref[...] = total.astype(jnp.bfloat16)

    def far_copy(k):
        return remote(rows.at[k, mine], rows.at[k, mine], far_sem, k, {"tp": far})

    def near_copy(k):
        return remote(rows.at[k, mine], rows.at[k, mine], near_sem, k, {"tp": near})

    def relay_copy(k):
        return remote(rows.at[k, theirs], rows.at[k, theirs], relay_sem, k, {"tp": near})

    def near_part_copy(k):
        span = pl.ds(pl.multiple_of((1 - core) * 2 * cap, 2 * cap), 2 * cap)
        return remote(part.at[k, span], near_part.at[k], np_sem, k, {"tp": near})

    def far_part_copy(k):
        return remote(pair_sum.at[k], far_part.at[k], fp_sem, k, {"tp": far})

    def return_copy(k):
        return remote(result.at[k], ret_ref.at[k], r_sem, k, behind(k))

    barrier = pltpu.get_barrier_semaphore()

    @pl.loop(1, ep)
    def _(k):
        pl.semaphore_signal(barrier, inc=1, device_id=ahead(k), device_id_type=MESH)

    for target in (near, far, across):
        pl.semaphore_signal(barrier, inc=1, device_id={"tp": target}, device_id_type=MESH)
    own_copy.start()
    pl.semaphore_wait(barrier, ep + 2)

    @pl.when(ep > 1)
    def _():
        z_copy(1).start()

    own_copy.wait()
    far_copy(0).start()
    near_copy(0).start()

    @pl.loop(0, tiles)
    def _(i):
        for copy in weight_copies(i):
            copy.start()

    down_copy.start()
    mix_copy.start()
    local_part()

    @pl.when(e == 0)
    def _():
        state_in[...] = jnp.zeros_like(state_in)
        if ep > 1:
            pass_state()

    def feed_forward(k):
        @pl.loop(0, tiles)
        def _(i):
            both = jnp.dot(rows[k], gate_up[i], preferred_element_type=jnp.float32)
            act, up_act = both[:, :LANES], both[:, LANES:]
            hidden[:, pl.ds(pl.multiple_of(i * LANES, LANES), LANES)] = (
                jax.nn.silu(act) * up_act
            ).astype(jnp.bfloat16)

        @pl.when(k == 0)
        def _():
            down_copy.wait()

        @pl.loop(0, width // 256)
        def _(i):
            cols = pl.ds(pl.multiple_of(i * 256, 256), 256)
            part[k, :, cols] = jnp.dot(
                hidden[...], down[:, cols], preferred_element_type=jnp.float32
            ).astype(jnp.bfloat16)

    def pair_stage(k):
        near_part_copy(k).wait_recv()
        other = pl.ds(pl.multiple_of((1 - side) * cap, cap), cap)
        pair_sum[k] = (
            part[k, theirs].astype(jnp.float32) + near_part[k, other].astype(jnp.float32)
        ).astype(jnp.bfloat16)
        far_part_copy(k).start()

    def final_stage(k):
        far_part_copy(k).wait_recv()
        own = pl.ds(pl.multiple_of(side * cap, cap), cap)
        total = (
            part[k, mine].astype(jnp.float32)
            + near_part[k, own].astype(jnp.float32)
            + far_part[k].astype(jnp.float32)
        ).astype(jnp.bfloat16)

        @pl.when(k == 0)
        def _():
            ret_ref[k] = total

        @pl.when(k > 0)
        def _():
            result[k] = total
            return_copy(k).start()

    @pl.loop(0, ep + 1)
    def _(k):
        @pl.when(k >= 1)
        def _():
            pair_stage(k - 1)

        @pl.when(k < ep)
        def _():
            far_copy(k).wait_recv()
            relay_copy(k).start()

        @pl.when(k + 1 < ep)
        def _():
            z_copy(k + 1).wait_recv()
            far_copy(k + 1).start()
            near_copy(k + 1).start()

        @pl.when(k + 2 < ep)
        def _():
            z_copy(k + 2).start()

        @pl.when(k == 0)
        def _():
            @pl.loop(0, tiles)
            def _(i):
                for copy in weight_copies(i):
                    copy.wait()

        @pl.when(k < ep)
        def _():
            near_copy(k).wait_recv()
            relay_copy(k).wait_recv()
            feed_forward(k)
            near_part_copy(k).start()

        @pl.when((k > 0) & (e == k))
        def _():
            state_copy.wait_recv()

            @pl.when(e + 1 < ep)
            def _():
                pass_state()

        @pl.when((k < ep) & (e == k))
        def _():
            memory_part()

        @pl.when(k >= 1)
        def _():
            final_stage(k - 1)

    mix_part()
    for i in range(3):
        memory_copy(i).wait_send()

    @pl.when(e + 1 < ep)
    def _():
        state_copy.wait_send()

    @pl.loop(0, ep)
    def _(k):
        far_copy(k).wait_send()
        near_copy(k).wait_send()
        relay_copy(k).wait_send()
        near_part_copy(k).wait_send()
        far_part_copy(k).wait_send()

    @pl.loop(1, ep)
    def _(k):
        z_copy(k).wait_send()

        return_copy(k).wait()


def expert_exchange(outgoing, memory_args, mix_weight, gate, up, down):
    ep, tp = lax.axis_size("ep"), lax.axis_size("tp")
    _, cap, width = outgoing.shape
    part_hidden = gate.shape[2]
    tiles = part_hidden // LANES
    bf16 = jnp.bfloat16
    vmem = pl.BlockSpec(memory_space=pltpu.VMEM)
    hbm = pl.BlockSpec(memory_space=pl.ANY)
    pair = pltpu.SemaphoreType.DMA((2, ep))
    rows = ep * tp * cap
    positions = memory_args[0].shape[0]
    heads = memory_args[3].shape[0]
    state = pltpu.VMEM((heads, DH + 8, DH), jnp.float32)
    return pl.pallas_call(
        functools.partial(expert_kernel, ep, tp, cap),
        out_shape=(
            jax.ShapeDtypeStruct(outgoing.shape, bf16),
            jax.ShapeDtypeStruct((positions, mix_weight.shape[1]), bf16),
        ),
        in_specs=[vmem] * 7 + [hbm] * 4,
        out_specs=(vmem, vmem),
        scratch_shapes=[
            pltpu.VMEM((tiles, width, 2 * LANES), bf16),
            pltpu.VMEM((part_hidden, width), bf16),
            pltpu.VMEM((ep, tp * cap, width), bf16),
            pltpu.VMEM((tp * cap, part_hidden), bf16),
            pltpu.VMEM((ep, tp * cap, width), bf16),
            pltpu.VMEM((ep, 2 * cap, width), bf16),
            pltpu.VMEM((ep, cap, width), bf16),
            pltpu.VMEM((ep, cap, width), bf16),
            pltpu.VMEM((ep, cap, width), bf16),
            state,
            state,
            state,
            pltpu.VMEM((tp, positions, heads * DH), bf16),
            pltpu.VMEM(mix_weight.shape, bf16),
            pltpu.SemaphoreType.DMA((2, tiles)),
            pltpu.SemaphoreType.DMA((3,)),
        ]
        + [pair] * 8
        + [pltpu.SemaphoreType.DMA((2, 3))],
        compiler_params=pltpu.CompilerParams(
            collective_id=0, has_side_effects=True, vmem_limit_bytes=66000000
        ),
        cost_estimate=pl.CostEstimate(
            flops=6 * rows * width * part_hidden, bytes_accessed=6 * width * part_hidden,
            transcendentals=rows * part_hidden,
        ),
    )(outgoing, *memory_args, mix_weight, gate, up, down)


def route_slots(routing_expert_index, experts, stride):
    flat_ids = routing_expert_index.reshape(-1)
    order = jnp.arange(flat_ids.shape[0], dtype=jnp.int32)
    earlier = (flat_ids[:, None] == flat_ids[None, :]) & (order[None, :] < order[:, None])
    route_ranks = jnp.sum(earlier.astype(jnp.int32), axis=1)
    turn = lax.rem(flat_ids + experts - lax.axis_index("ep"), experts)
    return (turn * stride + route_ranks).reshape(routing_expert_index.shape)


def on_device(
    memory_query_rows,
    memory_key_rows,
    memory_value_rows,
    input_gate_log,
    forget_gate_logits,
    forget_log_extra,
    memory_output_weight,
    second_batch_tokens,
    expert_norm_gain,
    routing_expert_index,
    routing_expert_weight,
    expert_gate_matrix,
    expert_up_matrix,
    expert_down_matrix,
):
    tok_rows = second_batch_tokens.shape[0]
    experts = lax.axis_size("ep")
    capacity = max(2, 5 * tok_rows * TOP // (4 * experts))
    stride = -(-capacity // 16) * 16
    slots_dev = experts * stride
    tokens_f = second_batch_tokens.astype(jnp.float32)
    normed = (
        tokens_f
        * lax.rsqrt(jnp.mean(tokens_f * tokens_f, axis=1, keepdims=True) + rms_eps)
        * expert_norm_gain
    ).astype(jnp.bfloat16)
    slot_ids = route_slots(routing_expert_index, experts, stride)
    slot_table = jnp.arange(slots_dev, dtype=jnp.int32)
    placing = jnp.zeros((slots_dev, tok_rows), jnp.bfloat16)
    for column in range(TOP):
        placing = placing + (slot_table[:, None] == slot_ids[None, :, column]).astype(jnp.bfloat16)
    outgoing = jnp.dot(placing, normed, preferred_element_type=jnp.float32).astype(jnp.bfloat16)
    returned, mixed_out = expert_exchange(
        outgoing.reshape(experts, stride, -1),
        (
            memory_query_rows,
            memory_key_rows,
            memory_value_rows,
            input_gate_log,
            forget_gate_logits,
            forget_log_extra,
        ),
        memory_output_weight,
        expert_gate_matrix,
        expert_up_matrix,
        expert_down_matrix,
    )
    choosing = jnp.zeros((tok_rows, slots_dev), jnp.float32)
    for column in range(TOP):
        choosing = choosing + jnp.where(
            slot_table[None, :] == slot_ids[:, column : column + 1],
            routing_expert_weight[:, column : column + 1],
            0.0,
        )
    expert_out = jnp.dot(
        choosing, returned.reshape(slots_dev, -1).astype(jnp.float32), precision=lax.Precision.HIGH
    ).astype(jnp.bfloat16)
    return (mixed_out, expert_out)


def solution(mesh):
    placed = (
        P(("grp", "ep"), "tp"),
        P(("grp", "ep"), "tp"),
        P(("grp", "ep"), "tp"),
        P("tp", ("grp", "ep")),
        P("tp", ("grp", "ep")),
        P("tp", ("grp", "ep")),
        P(None, "tp"),
        P(("grp", "ep", "tp"), None),
        P(),
        P(("grp", "ep", "tp"), None),
        P(("grp", "ep", "tp"), None),
        P("ep", None, "tp"),
        P("ep", None, "tp"),
        P("ep", "tp", None),
    )
    return jax.shard_map(
        on_device,
        mesh=mesh,
        in_specs=placed,
        out_specs=(P(("grp", "ep"), "tp"), P(("grp", "ep", "tp"), None)),
        check_vma=False,
    )
```
